32 devices in a mesh: ep: 16 (over z, y, x), tp: 2 (over core).
Axes of the slice: x: 2, y: 2, z: 4, core: 2. Of those that a mesh axis runs over, the one named last changes fastest.
Arguments:
- tokens: bfloat16 [512, 2048], P('ep'), may hold values from -6 to 6
- lru_state: float32 [512, 1024], P('ep', 'tp'), may hold values from -6 to 6
- conv_window: bfloat16 [512, 3, 1024], P('ep', None, 'tp'), may hold values from -6 to 6
- gain_mix_in: float32 [2048], replicated, may hold values from 0.1 to 1.9
- gain_mix_out: float32 [2048], replicated, may hold values from 0.1 to 1.9
- gain_ffn_in: float32 [2048], replicated, may hold values from 0.1 to 1.9
- gain_ffn_out: float32 [2048], replicated, may hold values from 0.1 to 1.9
- w_branch: bfloat16 [2048, 1024], P(None, 'tp'), may hold values from -0.125 to 0.125
- w_input: bfloat16 [2048, 1024], P(None, 'tp'), may hold values from -0.125 to 0.125
- conv_taps: bfloat16 [4, 1024], P(None, 'tp'), may hold values from -3 to 3
- gate_a: bfloat16 [8, 128, 128], P('tp'), may hold values from -0.5 to 0.5
- gate_x: bfloat16 [8, 128, 128], P('tp'), may hold values from -0.5 to 0.5
- decay_rate: float32 [1024], P('tp'), may hold values from 0.001 to 0.3
- w_mix_out: bfloat16 [1024, 2048], P('tp'), may hold values from -0.1875 to 0.1875
- routes: int32 [512, 4], P('ep'), may hold values from 0 to 15, all different within a row; in each aligned block of 32 rows (0 to 31, 32 to 63, ...) at most 16 rows name the same one
- route_weight: float32 [512, 4], P('ep'), may hold values from 0.2 to 1.5
- expert_gate: bfloat16 [16, 2048, 512], P('ep', None, 'tp'), may hold values from -0.125 to 0.125
- expert_up: bfloat16 [16, 2048, 512], P('ep', None, 'tp'), may hold values from -0.125 to 0.125
- expert_down: bfloat16 [16, 512, 2048], P('ep', 'tp'), may hold values from -0.25 to 0.25
- shared_gate: bfloat16 [2048, 512], P(None, 'tp'), may hold values from -0.125 to 0.125
- shared_up: bfloat16 [2048, 512], P(None, 'tp'), may hold values from -0.125 to 0.125
- shared_down: bfloat16 [512, 2048], P('tp'), may hold values from -0.25 to 0.25
Outputs:
- layer_out: bfloat16 [512, 2048], P('ep')
- new_state: float32 [512, 1024], P('ep', 'tp')
- new_window: bfloat16 [512, 3, 1024], P('ep', None, 'tp')
The draws below stay inside these ranges and needn't reach their ends.
Inputs may be any that keep to these rules, and one draw needn't show every extreme that they name: `routes`: each row names 4 different experts. Within the rows of one device (aligned blocks of 32 rows) no expert is named by more than 16 entries, a bound that some block reaches.
All inputs are finite; a program needn't handle non-finite values.
Results may differ from the reference program's by a relative error of at most 0.014.
Values may be sent and summed in bfloat16 or wider, within the bound.
A program may use at most 64 MiB of HBM per device.

```python
import math
import jax
import jax.numpy as jnp
import numpy as np
from jax import lax

D = 2048
DL = 1024
LRU_BLOCKS = 8
BD = 128
CONV_W = 4
FE = 512
SH = 512
TOP_K = 4
EXP_DEV = 1
EXPERTS = 16
SEQ_DEV = 32
TOKENS = 512
CAP = 16
N_EP = 16
N_TP = 2


def shard_levels(own_key, extent, pieces, smallest, largest):
    def one(position, parts):
        heights = jax.random.uniform(jax.random.fold_in(jax.random.fold_in(own_key, 6), position), (parts,), jnp.float32, smallest / len(pieces), largest / len(pieces))
        return jnp.repeat(jnp.exp(heights), extent[position] // parts).reshape((-1,) + (1,) * (len(extent) - position - 1))

    level = one(*pieces[0])
    for cut in pieces[1:]:
        level = level * one(*cut)
    return level


def assign_block(key, own, number, rows, count, top, most, lean):
    sequence = jax.random.permutation(key, count)
    heavy_load, usual = portions_of(count, rows * top, most, lean, True), portions_of(count, rows * top, most, lean, False)
    places = jnp.arange(count)

    def named(tallies, turn):
        used = int((tallies > 0).sum())
        fixed = max(1, used // 4)
        passed = fixed + (places - fixed + turn * (used - fixed)) % max(1, count - fixed)
        return jnp.zeros((count,), jnp.int32).at[sequence[jnp.where(places < fixed, places, passed)]].set(jnp.asarray(tallies, jnp.int32))

    tallies = jnp.where(number % 4 == 0, named(heavy_load, number // 4), named(usual, number - number // 4 - 1))
    mixed = jax.random.permutation(jax.random.fold_in(own, 3), count)
    giver, receiver = mixed[0:count // 2 * 2:2], mixed[1:count // 2 * 2:2]
    room = jnp.minimum(tallies[giver] - 1, most - tallies[receiver]) // 2
    room = jnp.where((giver == sequence[0]) | (receiver == sequence[0]) | (tallies[receiver] == 0), 0, jnp.maximum(room, 0))
    passed = jax.random.randint(jax.random.fold_in(own, 4), (count // 2,), 0, 1 << 20) % (room + 1)
    tallies = tallies.at[giver].add(-passed).at[receiver].add(passed)
    items = jnp.searchsorted(jnp.cumsum(tallies), jnp.arange(rows * top), side="right").astype(jnp.int32)
    table = items.reshape(top, rows).T
    table = table[jax.random.permutation(jax.random.fold_in(own, 1), rows)]
    turn = jax.random.randint(jax.random.fold_in(own, 2), (rows, 1), 0, top)
    return jnp.take_along_axis(table, (jnp.arange(top)[None, :] + turn) % top, axis=1)


def portions_of(number_of, total, bound, skew, full):
    portions = [(1 << 20) // math.isqrt(rank ** skew) + 1 for rank in range(1, number_of + 1)]
    largest = bound if full else min(bound, max(-(-total // number_of), total * portions[0] // sum(portions)))
    least = 1 if total - largest >= number_of - 1 else 0
    holding, spare = [largest] + [least] * (number_of - 1), total - largest - least * (number_of - 1)
    while spare > 0:
        free = [i for i in range(1, number_of) if holding[i] < largest] or [i for i in range(1, number_of) if holding[i] < bound]
        pool, remaining = sum([portions[i] for i in free]), spare
        for i in free:
            more = min(bound - holding[i], max(1, remaining * portions[i] // pool), spare)
            holding[i] = holding[i] + more
            spare = spare - more
    return np.array(holding)


def scatter_about(stream_key, shape, scale, most, shards=(), kind=jnp.bfloat16):
    values = jax.random.normal(stream_key, shape, jnp.float32) * scale
    if len(shards) > 0:
        values = shard_levels(stream_key, shape, shards, -0.22, 0.18) * values
    return jnp.clip(values, min=-most, max=most).astype(kind)


def setup_inputs(seed: int = 0) -> dict:
    streams_of = jax.random.split(jax.random.key(seed), 23)
    tokens = scatter_about(streams_of[0], (TOKENS, D), 1.0, 6.0, ((0, 16),))
    lru_state = scatter_about(streams_of[1], (TOKENS, DL), 1.0, 6.0, ((0, 16), (1, 2)), jnp.float32)
    conv_window = scatter_about(streams_of[2], (TOKENS, CONV_W - 1, DL), 1.0, 6.0, ((0, 16), (2, 2)))
    gain_mix_in = jnp.clip(1.0 + 0.18 * jax.random.normal(streams_of[3], (D,), jnp.float32), 0.1, 1.9)
    gain_mix_out = jnp.clip(1.0 + 0.18 * jax.random.normal(streams_of[4], (D,), jnp.float32), 0.1, 1.9)
    gain_ffn_in = jnp.clip(1.0 + 0.18 * jax.random.normal(streams_of[5], (D,), jnp.float32), 0.1, 1.9)
    gain_ffn_out = jnp.clip(1.0 + 0.18 * jax.random.normal(streams_of[6], (D,), jnp.float32), 0.1, 1.9)
    w_branch = scatter_about(streams_of[7], (D, DL), D ** -0.5, 0.125, ((1, 2),))
    w_input = scatter_about(streams_of[8], (D, DL), D ** -0.5, 0.125, ((1, 2),))
    conv_taps = scatter_about(streams_of[9], (CONV_W, DL), 0.5, 3.0, ((1, 2),))
    gate_a = scatter_about(streams_of[10], (LRU_BLOCKS, BD, BD), BD ** -0.5, 0.5, ((0, 2),))
    gate_x = scatter_about(streams_of[11], (LRU_BLOCKS, BD, BD), BD ** -0.5, 0.5, ((0, 2),))
    decay_rate = jnp.clip(jnp.exp(math.log(0.3) - 5.7037825 * jax.random.uniform(streams_of[12], (DL,), jnp.float32) ** shard_levels(streams_of[12], (DL,), ((0, 2),), -0.2, 0.2)), 0.001, 0.3)
    w_mix_out = scatter_about(streams_of[13], (DL, D), DL ** -0.5, 0.1875, ((0, 2),))
    routes_keys = jax.random.split(jax.random.fold_in(streams_of[14], 1), TOKENS // SEQ_DEV)
    routes_turns = jax.random.permutation(jax.random.fold_in(streams_of[14], 3), TOKENS // SEQ_DEV)
    routes = jax.vmap(lambda own, number: assign_block(jax.random.fold_in(streams_of[14], 2), own, number, SEQ_DEV, EXP_DEV * N_EP, TOP_K, CAP, 2))(routes_keys, routes_turns).reshape((TOKENS, TOP_K))
    route_weight = jnp.clip(jnp.exp(math.log(1.5) - 2.014903 * jax.random.uniform(streams_of[15], (TOKENS, TOP_K), jnp.float32) ** shard_levels(streams_of[15], (TOKENS, TOP_K), ((0, 16),), -0.2, 0.2)), 0.2, 1.5)
    expert_gate = scatter_about(streams_of[16], (EXPERTS, D, FE), D ** -0.5, 0.125, ((0, 16), (2, 2)))
    expert_up = scatter_about(streams_of[17], (EXPERTS, D, FE), D ** -0.5, 0.125, ((0, 16), (2, 2)))
    expert_down = scatter_about(streams_of[18], (EXPERTS, FE, D), FE ** -0.5, 0.25, ((0, 16), (1, 2)))
    shared_gate = scatter_about(streams_of[19], (D, SH), D ** -0.5, 0.125, ((1, 2),))
    shared_up = scatter_about(streams_of[20], (D, SH), D ** -0.5, 0.125, ((1, 2),))
    shared_down = scatter_about(streams_of[21], (SH, D), SH ** -0.5, 0.25, ((0, 2),))
    return dict(tokens=tokens, lru_state=lru_state, conv_window=conv_window, gain_mix_in=gain_mix_in, gain_mix_out=gain_mix_out, gain_ffn_in=gain_ffn_in, gain_ffn_out=gain_ffn_out, w_branch=w_branch, w_input=w_input, conv_taps=conv_taps, gate_a=gate_a, gate_x=gate_x, decay_rate=decay_rate, w_mix_out=w_mix_out, routes=routes, route_weight=route_weight, expert_gate=expert_gate, expert_up=expert_up, expert_down=expert_down, shared_gate=shared_gate, shared_up=shared_up, shared_down=shared_down)


def rms_norm(value, gain):
    return value * lax.rsqrt(lax.optimization_barrier(jnp.mean(value * value, axis=-1, keepdims=True)) + 1e-06) * gain

def parted(hidden, weight):
    width = hidden.shape[1]
    step = width // N_TP
    total = jnp.zeros((hidden.shape[0], weight.shape[1]), jnp.float32)
    for part in range(N_TP):
        piece = jnp.dot(hidden[:, part * step:(part + 1) * step], weight[part * step:(part + 1) * step], preferred_element_type=jnp.float32).astype(jnp.bfloat16)
        piece = lax.optimization_barrier(piece)
        total = total + piece.astype(jnp.float32)
    return total

def reference(tokens, lru_state, conv_window, gain_mix_in, gain_mix_out, gain_ffn_in, gain_ffn_out, w_branch, w_input, conv_taps, gate_a, gate_x, decay_rate, w_mix_out, routes, route_weight, expert_gate, expert_up, expert_down, shared_gate, shared_up, shared_down):
    resid = tokens.astype(jnp.float32)
    normed = rms_norm(resid, gain_mix_in).astype(jnp.bfloat16)
    branch = jnp.dot(normed, w_branch, preferred_element_type=jnp.float32)
    inflow = jnp.dot(normed, w_input, preferred_element_type=jnp.float32).astype(jnp.bfloat16)
    window = jnp.concatenate([conv_window, inflow[:, None, :]], axis=1)
    new_window = window[:, 1:]
    conv = lax.optimization_barrier(jnp.sum(window.astype(jnp.float32) * conv_taps.astype(jnp.float32)[None], axis=1))
    count = conv.shape[0]
    grouped = conv.astype(jnp.bfloat16).astype(jnp.float32).reshape(count, LRU_BLOCKS, BD)
    recur_gate = jax.nn.sigmoid(jnp.einsum('sbi,bij->sbj', grouped, gate_a.astype(jnp.float32)).reshape(count, DL))
    input_gate = jax.nn.sigmoid(jnp.einsum('sbi,bij->sbj', grouped, gate_x.astype(jnp.float32)).reshape(count, DL))
    log_decay = -8.0 * recur_gate * decay_rate[None]
    new_state = jnp.exp(log_decay) * lru_state + jnp.sqrt(-jnp.expm1(2.0 * log_decay)) * conv * input_gate
    gated = (new_state * jax.nn.gelu(branch)).astype(jnp.bfloat16)
    mixed = parted(gated, w_mix_out)
    middle = (resid + rms_norm(mixed, gain_mix_out)).astype(jnp.bfloat16)
    ffn_in = rms_norm(middle.astype(jnp.float32), gain_ffn_in).astype(jnp.bfloat16)
    shared_hidden = (jax.nn.silu(jnp.dot(ffn_in, shared_gate, preferred_element_type=jnp.float32)) * jnp.dot(ffn_in, shared_up, preferred_element_type=jnp.float32)).astype(jnp.bfloat16)
    shared = parted(shared_hidden, shared_down)
    per_block = SEQ_DEV * TOP_K
    flat = routes.reshape(N_EP, per_block)
    onehot = (flat[:, :, None] == jnp.arange(EXPERTS, dtype=jnp.int32)[None, None, :]).astype(jnp.int32)
    rank = lax.optimization_barrier(jnp.sum(onehot * (jnp.cumsum(onehot, axis=1) - 1), axis=-1))
    places = N_EP * CAP
    block_id = jnp.arange(N_EP, dtype=jnp.int32)[:, None]
    dest = (flat * places + block_id * CAP + rank).astype(jnp.int32)
    source = (block_id * SEQ_DEV + jnp.arange(per_block, dtype=jnp.int32)[None, :] // TOP_K).astype(jnp.int32)
    table = jnp.full((EXPERTS * places,), TOKENS, jnp.int32).at[dest.reshape(-1)].set(source.reshape(-1))
    table = table.reshape(EXPERTS, places)
    padded = jnp.concatenate([ffn_in, jnp.zeros((1, D), jnp.bfloat16)], axis=0)

    def one_expert(item):
        index, weight_g, weight_u, weight_d = item
        rows = padded[index]
        hidden = (jax.nn.silu(jnp.dot(rows, weight_g, preferred_element_type=jnp.float32)) * jnp.dot(rows, weight_u, preferred_element_type=jnp.float32)).astype(jnp.bfloat16)
        return parted(hidden, weight_d).astype(jnp.bfloat16)
    expert_out = lax.map(one_expert, (table, expert_gate, expert_up, expert_down))
    picked = expert_out.reshape(EXPERTS * places, D)[dest.reshape(-1)].reshape(TOKENS, TOP_K, D)
    routed = lax.optimization_barrier(jnp.sum(picked.astype(jnp.float32) * route_weight[:, :, None], axis=1)).astype(jnp.bfloat16)
    total = routed.astype(jnp.float32) + shared
    layer_out = (middle.astype(jnp.float32) + rms_norm(total, gain_ffn_out)).astype(jnp.bfloat16)
    return (layer_out, new_state, new_window)
```

```python
import functools

import jax
import jax.numpy as jnp
from jax import lax
from jax.experimental import pallas as pl
from jax.experimental.pallas import tpu as pltpu
from jax.sharding import PartitionSpec as P

F32 = jnp.float32
BF16 = jnp.bfloat16


def rms_norm(value, gain):
    return value * lax.rsqrt(jnp.mean(value * value, axis=-1, keepdims=True) + 1e-06) * gain


def dot(a, b):
    return jnp.dot(a, b, preferred_element_type=F32)


def one_less_exp(value):
    series = 1.0 + value * (1.0 / 6.0)
    for term in (5.0, 4.0, 3.0, 2.0):
        series = 1.0 + value * (1.0 / term) * series
    return jnp.where(value > -0.1, -value * series, 1.0 - jnp.exp(value))


def kernel(
    n_ep,
    cap,
    tokens_h,
    lru_h,
    cw_h,
    g_mix_in,
    g_mix_out,
    g_ffn_in,
    g_ffn_out,
    wb_h,
    wi_h,
    taps,
    ga_h,
    gx_h,
    decay_rate,
    wm_h,
    routes,
    route_w,
    eg_h,
    eu_h,
    ed_h,
    sg_h,
    su_h,
    sd_h,
    out_ref,
    state_ref,
    inflow_ref,
    tokens,
    lru,
    cw,
    wb,
    wi,
    ga,
    gx,
    wm,
    eg,
    eu,
    ed,
    sg,
    su,
    sd,
    mix_mine,
    mix_other,
    sh_mine,
    sh_other,
    ffn,
    outb,
    rows,
    part,
    part_in,
    ret,
    back,
    routed,
    load_sem,
    pair_send,
    pair_recv,
    ep_send,
    ep_recv,
    fwd_send,
    fwd_recv,
    ret_send,
    ret_recv,
):
    me = lax.axis_index("ep")
    tp = lax.axis_index("tp")
    other = 1 - tp
    partner = {"tp": other}
    count, width = tokens.shape
    share = width // 2
    slots = n_ep * cap
    chunk = min(slots, 256)
    chunks = slots // chunk

    barrier = pltpu.get_barrier_semaphore()
    pl.semaphore_signal(barrier, inc=1, device_id=partner, device_id_type=pl.DeviceIdType.MESH)

    def greet(i, carry):
        pl.semaphore_signal(
            barrier,
            inc=1,
            device_id={"ep": lax.rem(me + i, n_ep)},
            device_id_type=pl.DeviceIdType.MESH,
        )
        return carry

    lax.fori_loop(1, n_ep, greet, 0)

    loads = []
    for i, (src, dst) in enumerate(
        (
            (tokens_h, tokens),
            (wb_h, wb),
            (wi_h, wi),
            (cw_h, cw),
            (ga_h, ga),
            (gx_h, gx),
            (lru_h, lru),
            (wm_h, wm),
            (sg_h, sg),
            (su_h, su),
            (sd_h, sd),
            (eg_h, eg),
            (eu_h, eu),
            (ed_h, ed),
        )
    ):
        copy = pltpu.make_async_copy(src, dst, load_sem.at[i])
        copy.start()
        loads.append(copy)
    (c_tok, c_wb, c_wi, c_cw, c_ga, c_gx, c_lru, c_wm, c_sg, c_su, c_sd, c_eg, c_eu, c_ed) = loads

    tri = (
        lax.broadcasted_iota(jnp.int32, (count, count), 0)
        > lax.broadcasted_iota(jnp.int32, (count, count), 1)
    ).astype(BF16)

    def slot_maps(first):
        place = first + lax.broadcasted_iota(jnp.int32, (count, chunk), 1)
        expert = place // cap
        slot = (place - expert * cap).astype(F32)
        named = jnp.zeros((count, chunk), F32)
        weight = jnp.zeros((count, chunk), F32)
        for k in range(routes.shape[1]):
            hit = routes[:, k : k + 1] == expert
            named = jnp.where(hit, 1.0, named)
            weight = jnp.where(hit, route_w[:, k : k + 1], weight)
        rank = dot(tri, named.astype(BF16))
        filled = (rank == slot) & (named > 0.0)
        return jnp.where(filled, 1.0, 0.0), jnp.where(filled, weight, 0.0)

    def over_chunks(body):
        if chunks == 1:
            body(0)
        else:
            lax.fori_loop(0, chunks, lambda i, c: (body(pl.multiple_of(i * chunk, chunk)), c)[1], 0)

    one_map = slot_maps(0) if chunks == 1 else None

    c_tok.wait()
    resid = tokens[...].astype(F32)
    normed = rms_norm(resid, g_mix_in[...]).astype(BF16)
    c_wi.wait()
    inflow = dot(normed, wi[...]).astype(BF16)
    inflow_ref[...] = inflow
    c_wb.wait()
    branch = dot(normed, wb[...])
    c_cw.wait()
    tap = taps[...].astype(F32)
    conv = inflow.astype(F32) * tap[3:4]
    for j in range(3):
        conv = conv + cw[j].astype(F32) * tap[j : j + 1]
    low = conv.astype(BF16)
    c_ga.wait()
    c_gx.wait()
    groups, group = ga.shape[0], ga.shape[1]
    pre_a, pre_x = [], []
    for g in range(groups):
        piece = low[:, g * group : (g + 1) * group]
        pre_a.append(dot(piece, ga[g]))
        pre_x.append(dot(piece, gx[g]))
    recur_gate = jax.nn.sigmoid(jnp.concatenate(pre_a, axis=1))
    input_gate = jax.nn.sigmoid(jnp.concatenate(pre_x, axis=1))
    log_decay = -8.0 * recur_gate * decay_rate[...]
    c_lru.wait()
    new_state = (
        jnp.exp(log_decay) * lru[...] + jnp.sqrt(one_less_exp(2.0 * log_decay)) * conv * input_gate
    )
    state_ref[...] = new_state
    gated = (new_state * jax.nn.gelu(branch)).astype(BF16)
    c_wm.wait()
    mix_mine[...] = dot(gated, wm[...]).astype(BF16)

    def pair(i, src, dst):
        return pltpu.make_async_remote_copy(
            src_ref=src,
            dst_ref=dst,
            send_sem=pair_send.at[i],
            recv_sem=pair_recv.at[i],
            device_id=partner,
            device_id_type=pl.DeviceIdType.MESH,
        )

    pl.semaphore_wait(barrier, n_ep)
    mix_copy = pair(0, mix_mine, mix_other)
    mix_copy.start()
    mix_copy.wait()
    mixed = mix_mine[...].astype(F32) + mix_other[...].astype(F32)
    middle = (resid + rms_norm(mixed, g_mix_out[...])).astype(BF16)
    ffn_in = rms_norm(middle.astype(F32), g_ffn_in[...]).astype(BF16)
    ffn[0] = ffn_in[:, :share]
    ffn[1] = ffn_in[:, share:]

    def fill(first):
        place = (one_map or slot_maps(first))[0]
        own = ffn[tp]
        outb[pl.ds(first, chunk), :] = lax.dot_general(
            place.astype(BF16), own, (((0,), (0,)), ((), ())), preferred_element_type=F32
        ).astype(BF16)

    over_chunks(fill)

    def block(i):
        return pl.ds(pl.multiple_of(i * cap, cap), cap)

    def to_ep(i):
        peer = lax.rem(me + i, n_ep)
        return pltpu.make_async_remote_copy(
            src_ref=outb.at[block(peer), :],
            dst_ref=rows.at[tp, block(me), :],
            send_sem=ep_send.at[i],
            recv_sem=ep_recv.at[i],
            device_id={"ep": peer},
            device_id_type=pl.DeviceIdType.MESH,
        )

    def forward(i):
        peer = lax.rem(me + n_ep - i, n_ep)
        place = rows.at[tp, block(peer), :]
        return pltpu.make_async_remote_copy(
            src_ref=place,
            dst_ref=place,
            send_sem=fwd_send.at[i],
            recv_sem=fwd_recv.at[i],
            device_id=partner,
            device_id_type=pl.DeviceIdType.MESH,
        )

    lax.fori_loop(1, n_ep, lambda i, c: (to_ep(i).start(), c)[1], 0)
    rows[tp, block(me), :] = outb[block(me), :]
    forward(0).start()

    c_sg.wait()
    c_su.wait()
    hidden = (jax.nn.silu(dot(ffn_in, sg[...])) * dot(ffn_in, su[...])).astype(BF16)
    c_sd.wait()
    sh_mine[...] = dot(hidden, sd[...]).astype(BF16)
    sh_copy = pair(1, sh_mine, sh_other)
    sh_copy.start()

    def relay(i, c):
        to_ep(i).wait_recv()
        forward(i).start()
        return c

    lax.fori_loop(1, n_ep, relay, 0)
    lax.fori_loop(0, n_ep, lambda i, c: (forward(i).wait(), c)[1], 0)

    c_eg.wait()
    c_eu.wait()
    c_ed.wait()
    mine_at = pl.ds(pl.multiple_of(tp * share, share), share)
    other_at = pl.ds(pl.multiple_of(other * share, share), share)

    def expert(first):
        at = pl.ds(first, chunk)
        low_rows, high_rows = rows[0, at, :], rows[1, at, :]
        gate = dot(low_rows, eg[:share]) + dot(high_rows, eg[share:])
        up = dot(low_rows, eu[:share]) + dot(high_rows, eu[share:])
        act = (jax.nn.silu(gate) * up).astype(BF16)
        part[at, :] = dot(act, ed[:, other_at]).astype(BF16)
        ret[at, :] = dot(act, ed[:, mine_at]).astype(BF16)

    over_chunks(expert)
    part_copy = pair(2, part, part_in)
    part_copy.start()
    part_copy.wait()

    def add(first):
        at = pl.ds(first, chunk)
        ret[at, :] = (ret[at, :].astype(F32) + part_in[at, :].astype(F32)).astype(BF16)

    over_chunks(add)

    def to_back(i):
        peer = lax.rem(me + i, n_ep)
        return pltpu.make_async_remote_copy(
            src_ref=ret.at[block(peer), :],
            dst_ref=back.at[block(me), :],
            send_sem=ret_send.at[i],
            recv_sem=ret_recv.at[i],
            device_id={"ep": peer},
            device_id_type=pl.DeviceIdType.MESH,
        )

    lax.fori_loop(1, n_ep, lambda i, c: (to_back(i).start(), c)[1], 0)
    back[block(me), :] = ret[block(me), :]
    sh_copy.wait()
    shared = sh_mine[...].astype(F32) + sh_other[...].astype(F32)
    lax.fori_loop(1, n_ep, lambda i, c: (to_back(i).wait(), c)[1], 0)

    def combined(first):
        weight = (one_map or slot_maps(first))[1]
        high = weight.astype(BF16)
        rest = (weight - high.astype(F32)).astype(BF16)
        landed = back[pl.ds(first, chunk), :]
        return dot(high, landed) + dot(rest, landed)

    if chunks == 1:
        sums = combined(0)
    else:
        sums = lax.fori_loop(
            0,
            chunks,
            lambda i, c: c + combined(pl.multiple_of(i * chunk, chunk)),
            jnp.zeros((count, share), F32),
        )
    routed[tp] = sums.astype(BF16)
    routed_copy = pair(3, routed.at[tp], routed.at[tp])
    routed_copy.start()
    routed_copy.wait()
    total = jnp.concatenate([routed[0], routed[1]], axis=1).astype(F32) + shared
    out_ref[...] = (middle.astype(F32) + rms_norm(total, g_ffn_out[...])).astype(BF16)
    lax.fori_loop(1, n_ep, lambda i, c: (to_ep(i).wait_send(), c)[1], 0)


def on_device(
    tokens,
    lru_state,
    conv_window,
    gain_mix_in,
    gain_mix_out,
    gain_ffn_in,
    gain_ffn_out,
    w_branch,
    w_input,
    conv_taps,
    gate_a,
    gate_x,
    decay_rate,
    w_mix_out,
    routes,
    route_weight,
    expert_gate,
    expert_up,
    expert_down,
    shared_gate,
    shared_up,
    shared_down,
):
    n_ep = lax.axis_size("ep")
    count, width = tokens.shape
    share = width // 2
    local_ch = lru_state.shape[1]
    capacity = max(2, 2 * count * routes.shape[1] // (n_ep * expert_gate.shape[0]))
    cap = -(-capacity // 16) * 16
    slots = n_ep * cap
    vmem = pl.BlockSpec(memory_space=pltpu.VMEM)
    hbm = pl.BlockSpec(memory_space=pl.ANY)
    window = jnp.transpose(conv_window, (1, 0, 2))
    args = (
        (tokens, hbm),
        (lru_state, hbm),
        (window, hbm),
        (gain_mix_in[None], vmem),
        (gain_mix_out[None], vmem),
        (gain_ffn_in[None], vmem),
        (gain_ffn_out[None], vmem),
        (w_branch, hbm),
        (w_input, hbm),
        (conv_taps, vmem),
        (gate_a, hbm),
        (gate_x, hbm),
        (decay_rate[None], vmem),
        (w_mix_out, hbm),
        (routes, vmem),
        (route_weight, vmem),
        (expert_gate[0], hbm),
        (expert_up[0], hbm),
        (expert_down[0], hbm),
        (shared_gate, hbm),
        (shared_up, hbm),
        (shared_down, hbm),
    )
    held = lambda a: pltpu.VMEM(a.shape, a.dtype)
    dma = pltpu.SemaphoreType.DMA
    layer_out, new_state, inflow = pl.pallas_call(
        functools.partial(kernel, n_ep, cap),
        out_shape=(
            jax.ShapeDtypeStruct((count, width), BF16),
            jax.ShapeDtypeStruct((count, local_ch), F32),
            jax.ShapeDtypeStruct((count, local_ch), BF16),
        ),
        in_specs=[spec for _, spec in args],
        out_specs=(vmem, vmem, vmem),
        scratch_shapes=[
            held(tokens),
            held(lru_state),
            held(window),
            held(w_branch),
            held(w_input),
            held(gate_a),
            held(gate_x),
            held(w_mix_out),
            held(expert_gate[0]),
            held(expert_up[0]),
            held(expert_down[0]),
            held(shared_gate),
            held(shared_up),
            held(shared_down),
            pltpu.VMEM((count, width), BF16),
            pltpu.VMEM((count, width), BF16),
            pltpu.VMEM((count, width), BF16),
            pltpu.VMEM((count, width), BF16),
            pltpu.VMEM((2, count, share), BF16),
            pltpu.VMEM((slots, share), BF16),
            pltpu.VMEM((2, slots, share), BF16),
            pltpu.VMEM((slots, share), BF16),
            pltpu.VMEM((slots, share), BF16),
            pltpu.VMEM((slots, share), BF16),
            pltpu.VMEM((slots, share), BF16),
            pltpu.VMEM((2, count, share), BF16),
            dma((14,)),
            dma((4,)),
            dma((4,)),
            dma((n_ep,)),
            dma((n_ep,)),
            dma((n_ep,)),
            dma((n_ep,)),
            dma((n_ep,)),
            dma((n_ep,)),
        ],
        compiler_params=pltpu.CompilerParams(
            collective_id=0, has_side_effects=True, vmem_limit_bytes=60 * 1024 * 1024
        ),
        name="layer",
    )(*[value for value, _ in args])
    new_window = jnp.concatenate([conv_window[:, 1:], inflow[:, None, :]], axis=1)
    return (layer_out, new_state, new_window)


def solution(mesh):
    placed = (
        P("ep", None),
        P("ep", "tp"),
        P("ep", None, "tp"),
        P(),
        P(),
        P(),
        P(),
        P(None, "tp"),
        P(None, "tp"),
        P(None, "tp"),
        P("tp", None, None),
        P("tp", None, None),
        P("tp"),
        P("tp", None),
        P("ep", None),
        P("ep", None),
        P("ep", None, "tp"),
        P("ep", None, "tp"),
        P("ep", "tp", None),
        P(None, "tp"),
        P(None, "tp"),
        P("tp", None),
    )
    return jax.shard_map(
        on_device,
        mesh=mesh,
        in_specs=placed,
        out_specs=(P("ep", None), P("ep", "tp"), P("ep", None, "tp")),
        check_vma=False,
    )
```

```python
import functools

import jax
import jax.numpy as jnp
from jax import lax
from jax.experimental import pallas as pl
from jax.experimental.pallas import tpu as pltpu
from jax.sharding import PartitionSpec as P

F32 = jnp.float32
BF16 = jnp.bfloat16
MESH = pl.DeviceIdType.MESH


def rms_norm(value, gain):
    return value * lax.rsqrt(jnp.mean(value * value, axis=-1, keepdims=True) + 1e-06) * gain


def dot(a, b):
    return jnp.dot(a, b, preferred_element_type=F32)


def one_less_exp(value):
    series = 1.0 + value * (1.0 / 6.0)
    for term in (5.0, 4.0, 3.0, 2.0):
        series = 1.0 + value * (1.0 / term) * series
    return jnp.where(value > -0.1, -value * series, 1.0 - jnp.exp(value))


def kernel(
    outer,
    inner,
    cap,
    tokens_h,
    lru_h,
    cw_h,
    g_mix_in,
    g_mix_out,
    g_ffn_in,
    g_ffn_out,
    wb_h,
    wi_h,
    taps,
    ga_h,
    gx_h,
    decay_rate,
    wm_h,
    routes,
    route_w,
    eg_h,
    eu_h,
    ed_h,
    sg_h,
    su_h,
    sd_h,
    out_ref,
    state_ref,
    inflow_ref,
    tokens,
    lru,
    cw,
    wb,
    wi,
    ga,
    gx,
    wm,
    eg,
    eu,
    ed,
    sg,
    su,
    sd,
    mix_mine,
    mix_other,
    sh_mine,
    sh_other,
    ffn,
    info,
    line,
    outb,
    rows,
    part,
    part_in,
    kept,
    ret,
    back,
    sums,
    sums_in,
    own_sum,
    routed,
    load_sem,
    pair_send,
    pair_recv,
    ep_send,
    ep_recv,
    fwd_send,
    fwd_recv,
    ret_send,
    ret_recv,
    info_send,
    info_recv,
    line_send,
    line_recv,
    part_send,
    part_recv,
    sum_send,
    sum_recv,
):
    z, q = lax.axis_index("ep") // inner, lax.axis_index("ep") % inner
    tp = lax.axis_index("tp")
    other = 1 - tp
    partner = {"tp": other}
    count, width = tokens.shape
    share = width // 2
    order = sorted(range(1, outer), key=lambda j: -j)

    def from_z(j):
        place, bit = z, 1
        while bit <= j:
            if j & bit:
                place = place + bit - 2 * bit * (z // bit % 2)
            bit *= 2
        return place

    barrier = pltpu.get_barrier_semaphore()

    def greet(device):
        pl.semaphore_signal(barrier, inc=1, device_id=device, device_id_type=MESH)

    greet(partner)
    for j in range(1, outer):
        greet({"ep": from_z(j) * inner + q})
    lax.fori_loop(
        1, inner, lambda i, c: (greet({"ep": z * inner + lax.rem(q + i, inner)}), c)[1], 0
    )

    loads = []
    for i, (src, dst) in enumerate(
        (
            (tokens_h, tokens),
            (wb_h, wb),
            (wi_h, wi),
            (cw_h, cw),
            (ga_h, ga),
            (gx_h, gx),
            (lru_h, lru),
            (wm_h, wm),
            (sg_h, sg),
            (su_h, su),
            (sd_h, sd),
            (eg_h, eg),
            (eu_h, eu),
            (ed_h, ed),
        )
    ):
        copy = pltpu.make_async_copy(src, dst, load_sem.at[i])
        copy.start()
        loads.append(copy)
    (c_tok, c_wb, c_wi, c_cw, c_ga, c_gx, c_lru, c_wm, c_sg, c_su, c_sd, c_eg, c_eu, c_ed) = loads

    plane_rows = inner * cap
    earlier = (
        lax.broadcasted_iota(jnp.int32, (count, count), 0)
        < lax.broadcasted_iota(jnp.int32, (count, count), 1)
    ).astype(BF16)
    top = routes.shape[0]
    info[z] = jnp.zeros(info.shape[1:], F32)
    info[z, :top, :count] = routes[...].astype(F32)
    info[z, top : 2 * top, :count] = route_w[...]

    def slot_maps(block_z):
        place = lax.broadcasted_iota(jnp.int32, (plane_rows, count), 0)
        expert = place // cap
        slot = (place - expert * cap).astype(F32)
        expert = (expert + z * inner).astype(F32)
        named = jnp.zeros((plane_rows, count), F32)
        weight = jnp.zeros((plane_rows, count), F32)
        for k in range(top):
            hit = info[block_z, k : k + 1, :count] == expert
            named = jnp.where(hit, 1.0, named)
            weight = jnp.where(hit, info[block_z, top + k : top + k + 1, :count], weight)
        filled = (dot(named.astype(BF16), earlier) == slot) & (named > 0.0)
        return jnp.where(filled, 1.0, 0.0).astype(BF16), jnp.where(filled, weight, 0.0)

    c_tok.wait()
    resid = tokens[...].astype(F32)
    normed = rms_norm(resid, g_mix_in[...]).astype(BF16)
    c_wi.wait()
    inflow = dot(normed, wi[...]).astype(BF16)
    inflow_ref[...] = inflow
    c_wb.wait()
    branch = dot(normed, wb[...])
    c_cw.wait()
    tap = taps[...].astype(F32)
    conv = inflow.astype(F32) * tap[3:4]
    for j in range(3):
        conv = conv + cw[j].astype(F32) * tap[j : j + 1]
    low = conv.astype(BF16)
    c_ga.wait()
    c_gx.wait()
    groups, group = ga.shape[0], ga.shape[1]
    pre_a, pre_x = [], []
    for g in range(groups):
        piece = low[:, g * group : (g + 1) * group]
        pre_a.append(dot(piece, ga[g]))
        pre_x.append(dot(piece, gx[g]))
    recur_gate = jax.nn.sigmoid(jnp.concatenate(pre_a, axis=1))
    input_gate = jax.nn.sigmoid(jnp.concatenate(pre_x, axis=1))
    log_decay = -8.0 * recur_gate * decay_rate[...]
    c_lru.wait()
    new_state = (
        jnp.exp(log_decay) * lru[...] + jnp.sqrt(one_less_exp(2.0 * log_decay)) * conv * input_gate
    )
    state_ref[...] = new_state
    gated = (new_state * jax.nn.gelu(branch)).astype(BF16)
    c_wm.wait()
    mix_mine[...] = dot(gated, wm[...]).astype(BF16)

    def pair(i, src, dst):
        return pltpu.make_async_remote_copy(
            src_ref=src,
            dst_ref=dst,
            send_sem=pair_send.at[i],
            recv_sem=pair_recv.at[i],
            device_id=partner,
            device_id_type=MESH,
        )

    def on_line(src, dst, send, recv, j):
        return pltpu.make_async_remote_copy(
            src_ref=src.at[z],
            dst_ref=dst.at[z],
            send_sem=send.at[j],
            recv_sem=recv.at[j],
            device_id={"ep": from_z(j) * inner + q},
            device_id_type=MESH,
        )

    def info_copy(j):
        return on_line(info, info, info_send, info_recv, j)

    def line_copy(j):
        return on_line(line, line, line_send, line_recv, j)

    pl.semaphore_wait(barrier, outer + inner - 1)
    mix_copy = pair(0, mix_mine, mix_other)
    mix_copy.start()
    for j in order:
        info_copy(j).start()
    mix_copy.wait()
    mixed = mix_mine[...].astype(F32) + mix_other[...].astype(F32)
    middle = (resid + rms_norm(mixed, g_mix_out[...])).astype(BF16)
    ffn_in = rms_norm(middle.astype(F32), g_ffn_in[...]).astype(BF16)
    ffn[0] = ffn_in[:, :share]
    ffn[1] = ffn_in[:, share:]

    line[z] = ffn[tp]
    for j in order:
        line_copy(j).start()

    def block(i):
        return pl.ds(pl.multiple_of(i * cap, cap), cap)

    def at_plane(j, i):
        return block(from_z(j) * inner + lax.rem(i, inner))

    def to_ep(j, i):
        return pltpu.make_async_remote_copy(
            src_ref=outb.at[at_plane(j, q + i), :],
            dst_ref=rows.at[tp, at_plane(j, q), :],
            send_sem=ep_send.at[j * inner + i],
            recv_sem=ep_recv.at[j * inner + i],
            device_id={"ep": z * inner + lax.rem(q + i, inner)},
            device_id_type=MESH,
        )

    def forward(j, i):
        place = rows.at[tp, at_plane(j, q + inner - i), :]
        return pltpu.make_async_remote_copy(
            src_ref=place,
            dst_ref=place,
            send_sem=fwd_send.at[j * inner + i],
            recv_sem=fwd_recv.at[j * inner + i],
            device_id=partner,
            device_id_type=MESH,
        )

    def to_back(j, i):
        return pltpu.make_async_remote_copy(
            src_ref=ret.at[at_plane(j, q + i), :],
            dst_ref=back.at[at_plane(j, q), :],
            send_sem=ret_send.at[j * inner + i],
            recv_sem=ret_recv.at[j * inner + i],
            device_id={"ep": z * inner + lax.rem(q + i, inner)},
            device_id_type=MESH,
        )

    def rows_of(j):
        return pl.ds(pl.multiple_of(from_z(j) * plane_rows, plane_rows), plane_rows)

    def part_copy(j):
        return pltpu.make_async_remote_copy(
            src_ref=part.at[rows_of(j), :],
            dst_ref=part_in.at[rows_of(j), :],
            send_sem=part_send.at[j],
            recv_sem=part_recv.at[j],
            device_id=partner,
            device_id_type=MESH,
        )

    def sum_copy(j):
        return pltpu.make_async_remote_copy(
            src_ref=sums.at[j],
            dst_ref=sums_in.at[j],
            send_sem=sum_send.at[j],
            recv_sem=sum_recv.at[j],
            device_id={"ep": from_z(j) * inner + q},
            device_id_type=MESH,
        )

    def each(first, body):
        lax.fori_loop(first, inner, lambda i, c: (body(i), c)[1], 0)

    weights = {}

    def send_rows(j):
        if j > 0:
            info_copy(j).wait_recv()
            line_copy(j).wait_recv()
        place, weights[j] = slot_maps(from_z(j))
        outb[rows_of(j), :] = dot(place, line[from_z(j)]).astype(BF16)
        each(1, lambda i: to_ep(j, i).start())
        rows[tp, at_plane(j, q), :] = outb[at_plane(j, q), :]
        forward(j, 0).start()

    def relay_rows(j):
        def one(i):
            to_ep(j, i).wait_recv()
            forward(j, i).start()

        each(1, one)

    mine_at = pl.ds(pl.multiple_of(tp * share, share), share)
    other_at = pl.ds(pl.multiple_of(other * share, share), share)

    def run_expert(j):
        if j == 0:
            c_eg.wait()
            c_eu.wait()
            c_ed.wait()
        each(0, lambda i: forward(j, i).wait_recv())
        low_rows, high_rows = rows[0, rows_of(j), :], rows[1, rows_of(j), :]
        gate = dot(low_rows, eg[:share]) + dot(high_rows, eg[share:])
        up = dot(low_rows, eu[:share]) + dot(high_rows, eu[share:])
        act = (jax.nn.silu(gate) * up).astype(BF16)
        part[rows_of(j), :] = dot(act, ed[:, other_at]).astype(BF16)
        part_copy(j).start()
        kept[rows_of(j), :] = dot(act, ed[:, mine_at]).astype(BF16)

    def send_back(j):
        part_copy(j).wait_recv()
        ret[rows_of(j), :] = (
            kept[rows_of(j), :].astype(F32) + part_in[rows_of(j), :].astype(F32)
        ).astype(BF16)
        each(1, lambda i: to_back(j, i).start())
        back[at_plane(j, q), :] = ret[at_plane(j, q), :]

    def weigh(j):
        each(1, lambda i: to_back(j, i).wait_recv())
        high = weights[j].astype(BF16)
        rest = (weights[j] - high.astype(F32)).astype(BF16)
        landed = back[rows_of(j), :]
        turned = lambda w: lax.dot_general(
            w, landed, (((0,), (0,)), ((), ())), preferred_element_type=F32
        )
        partial = turned(high) + turned(rest)
        if j == 0:
            own_sum[...] = partial
        else:
            sums[j] = partial.astype(BF16)
            sum_copy(j).start()

    sh_copy = pair(1, sh_mine, sh_other)
    for step in range(outer + 5):
        for stage, lag in ((send_rows, 0), (send_back, 3), (run_expert, 2), (relay_rows, 1), (weigh, 5)):
            if 0 <= step - lag < outer:
                stage(step - lag)
        if step == 0:
            c_sg.wait()
            c_su.wait()
            hidden = (jax.nn.silu(dot(ffn_in, sg[...])) * dot(ffn_in, su[...])).astype(BF16)
            c_sd.wait()
            sh_mine[...] = dot(hidden, sd[...]).astype(BF16)
            sh_copy.start()

    sh_copy.wait()
    shared = sh_mine[...].astype(F32) + sh_other[...].astype(F32)
    routed_sum = own_sum[...]
    for j in range(1, outer):
        sum_copy(j).wait_recv()
        routed_sum = routed_sum + sums_in[j].astype(F32)
    routed[tp] = routed_sum.astype(BF16)
    routed_copy = pair(2, routed.at[tp], routed.at[tp])
    routed_copy.start()
    routed_copy.wait()
    total = jnp.concatenate([routed[0], routed[1]], axis=1).astype(F32) + shared
    out_ref[...] = (middle.astype(F32) + rms_norm(total, g_ffn_out[...])).astype(BF16)
    for j in range(outer):
        if j > 0:
            info_copy(j).wait_send()
            line_copy(j).wait_send()
            sum_copy(j).wait_send()
        part_copy(j).wait_send()
        each(0, lambda i: forward(j, i).wait_send())
        each(1, lambda i: to_ep(j, i).wait_send())
        each(1, lambda i: to_back(j, i).wait_send())


def tail(layer_out, state, inflow, window, out_ref, state_ref, window_ref):
    out_ref[...] = layer_out[...]
    state_ref[...] = state[...]
    taken = window.shape[0]
    for j in range(taken - 1):
        window_ref[j] = window[j + 1]
    window_ref[taken - 1] = inflow[...]


def on_device(
    tokens,
    lru_state,
    conv_window,
    gain_mix_in,
    gain_mix_out,
    gain_ffn_in,
    gain_ffn_out,
    w_branch,
    w_input,
    conv_taps,
    gate_a,
    gate_x,
    decay_rate,
    w_mix_out,
    routes,
    route_weight,
    expert_gate,
    expert_up,
    expert_down,
    shared_gate,
    shared_up,
    shared_down,
):
    n_ep = lax.axis_size("ep")
    count, width = tokens.shape
    share = width // 2
    local_ch = lru_state.shape[1]
    capacity = max(2, 2 * count * routes.shape[1] // (n_ep * expert_gate.shape[0]))
    cap = -(-capacity // 16) * 16
    slots = n_ep * cap
    outer = 1
    while outer * outer * 4 <= n_ep and n_ep % (2 * outer) == 0:
        outer *= 2
    inner = n_ep // outer
    vmem = pl.BlockSpec(memory_space=pltpu.VMEM)
    hbm = pl.BlockSpec(memory_space=pl.ANY)
    window = jnp.transpose(conv_window, (1, 0, 2))
    args = (
        (tokens, hbm),
        (lru_state, hbm),
        (window, hbm),
        (gain_mix_in[None], vmem),
        (gain_mix_out[None], vmem),
        (gain_ffn_in[None], vmem),
        (gain_ffn_out[None], vmem),
        (w_branch, hbm),
        (w_input, hbm),
        (conv_taps, vmem),
        (gate_a, hbm),
        (gate_x, hbm),
        (decay_rate[None], vmem),
        (w_mix_out, hbm),
        (routes.T, vmem),
        (route_weight.T, vmem),
        (expert_gate[0], hbm),
        (expert_up[0], hbm),
        (expert_down[0], hbm),
        (shared_gate, hbm),
        (shared_up, hbm),
        (shared_down, hbm),
    )
    held = lambda a: pltpu.VMEM(a.shape, a.dtype)
    dma = pltpu.SemaphoreType.DMA
    layer_out, new_state, inflow = pl.pallas_call(
        functools.partial(kernel, outer, inner, cap),
        out_shape=(
            jax.ShapeDtypeStruct((count, width), BF16),
            jax.ShapeDtypeStruct((count, local_ch), F32),
            jax.ShapeDtypeStruct((count, local_ch), BF16),
        ),
        in_specs=[spec for _, spec in args],
        out_specs=(vmem, vmem, vmem),
        scratch_shapes=[
            held(tokens),
            held(lru_state),
            held(window),
            held(w_branch),
            held(w_input),
            held(gate_a),
            held(gate_x),
            held(w_mix_out),
            held(expert_gate[0]),
            held(expert_up[0]),
            held(expert_down[0]),
            held(shared_gate),
            held(shared_up),
            held(shared_down),
            pltpu.VMEM((count, width), BF16),
            pltpu.VMEM((count, width), BF16),
            pltpu.VMEM((count, width), BF16),
            pltpu.VMEM((count, width), BF16),
            pltpu.VMEM((2, count, share), BF16),
            pltpu.VMEM((outer, -(-2 * routes.shape[1] // 8) * 8, -(-count // 128) * 128), F32),
            pltpu.VMEM((outer, count, share), BF16),
            pltpu.VMEM((slots, share), BF16),
            pltpu.VMEM((2, slots, share), BF16),
            pltpu.VMEM((slots, share), BF16),
            pltpu.VMEM((slots, share), BF16),
            pltpu.VMEM((slots, share), BF16),
            pltpu.VMEM((slots, share), BF16),
            pltpu.VMEM((slots, share), BF16),
            pltpu.VMEM((outer, count, share), BF16),
            pltpu.VMEM((outer, count, share), BF16),
            pltpu.VMEM((count, share), F32),
            pltpu.VMEM((2, count, share), BF16),
            dma((14,)),
            dma((3,)),
            dma((3,)),
            dma((n_ep,)),
            dma((n_ep,)),
            dma((n_ep,)),
            dma((n_ep,)),
            dma((n_ep,)),
            dma((n_ep,)),
        ]
        + [dma((outer,))] * 8,
        compiler_params=pltpu.CompilerParams(
            collective_id=0, has_side_effects=True, vmem_limit_bytes=60 * 1024 * 1024
        ),
        name="layer",
    )(*[value for value, _ in args])
    layer_out, new_state, new_window = pl.pallas_call(
        tail,
        out_shape=(
            jax.ShapeDtypeStruct((count, width), BF16),
            jax.ShapeDtypeStruct((count, local_ch), F32),
            jax.ShapeDtypeStruct(window.shape, BF16),
        ),
        in_specs=[vmem] * 4,
        out_specs=(vmem,) * 3,
        name="hand_over",
    )(layer_out, new_state, inflow, window)
    return (layer_out, new_state, jnp.transpose(new_window, (1, 0, 2)))


def solution(mesh):
    placed = (
        P("ep", None),
        P("ep", "tp"),
        P("ep", None, "tp"),
        P(),
        P(),
        P(),
        P(),
        P(None, "tp"),
        P(None, "tp"),
        P(None, "tp"),
        P("tp", None, None),
        P("tp", None, None),
        P("tp"),
        P("tp", None),
        P("ep", None),
        P("ep", None),
        P("ep", None, "tp"),
        P("ep", None, "tp"),
        P("ep", "tp", None),
        P(None, "tp"),
        P(None, "tp"),
        P("tp", None),
    )
    return jax.shard_map(
        on_device,
        mesh=mesh,
        in_specs=placed,
        out_specs=(P("ep", None), P("ep", "tp"), P("ep", None, "tp")),
        check_vma=False,
    )
```
